512 devices in a mesh: rep: 2 (over z_hi), fs: 32 (over z_lo, y), tp: 8 (over x, core).
Axes of the slice: x: 4, y: 4, z: 16 (z_hi: 2, z_lo: 8; z = z_hi * 8 + z_lo), core: 2. Of those that a mesh axis runs over, the one named last changes fastest.
Arguments:
- tokens: bfloat16 [49152, 2048], P(('rep', 'fs')), may hold values from -6 to 6
- norm_gain: float32 [2048], replicated, may hold values from 0.1 to 1.9
- up_weight: bfloat16 [2048, 8192], P('fs', 'tp'), may hold values from -0.125 to 0.125
- down_weight: bfloat16 [8192, 2048], P('tp', 'fs'), may hold values from -0.0625 to 0.0625
Outputs:
- layer_out: bfloat16 [49152, 2048], P(('rep', 'fs'), 'tp')
The draws below stay inside these ranges and needn't reach their ends.
All inputs are finite; a program needn't handle non-finite values.
Results may differ from the reference program's by a relative error of at most 0.013.
Values may be sent and summed in bfloat16 or wider, within the bound.
No kernel may reach another device: no remote copies, remote signals or barrier semaphores. Data moves between devices by JAX's collectives and lax.ppermute only.
A program may use at most 64 MiB of HBM per device.

```python
import jax
import jax.numpy as jnp
from jax import lax

D = 2048
FF = 8192
TOK_GRP = 768
TOKENS = 49152
N_REP = 2
N_FS = 32
N_TP = 8


def block_scale(own_key, extent, split, smallest, high):
    gain, own = 1.0, jax.random.fold_in(own_key, 6)
    for dim, parts in split:
        draws = jnp.exp(jax.random.uniform(jax.random.fold_in(own, dim), (parts,), jnp.float32, smallest / len(split), high / len(split)))
        gain = gain * jnp.repeat(draws, extent[dim] // parts).reshape([-1 if axis == dim else 1 for axis in range(len(extent))])
    return gain


def gaussian(key, shape, scale, bound, cuts=(), dtype=jnp.bfloat16):
    entries = jax.random.normal(key, shape, jnp.float32) * scale
    if len(cuts) > 0:
        entries = block_scale(key, shape, cuts, -0.22, 0.18) * entries
    return jnp.clip(entries, min=-bound, max=bound).astype(dtype)


def setup_inputs(seed: int = 0) -> dict:
    seeds = jax.random.split(jax.random.key(seed), 5)
    return {
        "tokens": gaussian(seeds[0], (TOKENS, D), 1.0, 6.0, ((0, 64),)),
        "norm_gain": jnp.clip(1.0 + 0.18 * jax.random.normal(seeds[1], (D,), jnp.float32), 0.1, 1.9),
        "up_weight": gaussian(seeds[2], (D, FF), D ** -0.5, 0.125, ((0, 32), (1, 8))),
        "down_weight": gaussian(seeds[3], (FF, D), FF ** -0.5, 0.0625, ((0, 8), (1, 32))),
    }


def group_layer(rows, norm_gain, up_weight, down_weight):
    xf = rows.astype(jnp.float32)
    inv_rms = lax.rsqrt(lax.optimization_barrier(jnp.mean(xf * xf, axis=-1, keepdims=True)) + 1e-06)
    normed = (xf * inv_rms * norm_gain).astype(jnp.bfloat16)
    pre = jnp.dot(normed, up_weight, preferred_element_type=jnp.float32)
    hidden = jnp.square(jax.nn.relu(pre)).astype(jnp.bfloat16)
    width = hidden.shape[1] // N_TP
    total = xf
    for block in range(N_TP):
        partial_value = jnp.dot(hidden[:, block * width:(block + 1) * width], down_weight[block * width:(block + 1) * width], preferred_element_type=jnp.float32)
        total = total + partial_value.astype(jnp.bfloat16).astype(jnp.float32)
    return total.astype(jnp.bfloat16)

def reference(tokens, norm_gain, up_weight, down_weight):
    groups = tokens.reshape(N_REP * N_FS, TOK_GRP, D)
    result = lax.map(lambda rows: group_layer(rows, norm_gain, up_weight, down_weight), groups)
    return result.reshape(TOKENS, D)
```

```python
import jax
import jax.numpy as jnp
from jax import lax
from jax.experimental import pallas as pl
from jax.experimental.pallas import tpu as pltpu
from jax.sharding import Mesh
from jax.sharding import PartitionSpec as P


AXES = ("r", "z", "y", "x", "c")
RING, NY, NX, NC = 16, 4, 4, 2
UNIT = 64


def device_number(zz, y, x, c):
    return ((zz % RING * NY + y % NY) * NX + x % NX) * NC + c % NC


def fetched(array, offset):
    pairs = []
    for zz in range(RING):
        for y in range(NY):
            for x in range(NX):
                for c in range(NC):
                    dz, dy, dx, dc = offset(c)
                    pairs.append((device_number(zz + dz, y + dy, x + dx, c + dc), device_number(zz, y, x, c)))
    return lax.ppermute(array, AXES, pairs)


def along_z(k):
    return lambda c: (-k if k == 2 and c == 1 else k, 0, 0, 0)


def along_y(k):
    return lambda c: (0, k, 0, 0)


def spread(top, bottom, step):
    next_top, before_bottom = fetched(top, step(1)), fetched(bottom, step(-1))
    next_bottom, before_top = fetched(bottom, step(1)), fetched(top, step(-1))
    far_top, far_bottom = fetched(next_top, step(1)), fetched(before_bottom, step(-1))
    return top, bottom, next_top, next_bottom, before_top, before_bottom, far_top, far_bottom


VMEM = pl.BlockSpec(memory_space=pltpu.VMEM)
SMEM = pl.BlockSpec(memory_space=pltpu.SMEM)


def local_call(kernel, shapes, operands, flops=0, scratch=(), tables=0, limit=8):
    return pl.pallas_call(
        kernel,
        out_shape=shapes,
        in_specs=[SMEM] * tables + [VMEM] * (len(operands) - tables),
        out_specs=jax.tree.map(lambda _: VMEM, shapes),
        scratch_shapes=list(scratch),
        compiler_params=pltpu.CompilerParams(vmem_limit_bytes=limit << 20),
        cost_estimate=pl.CostEstimate(flops=flops, bytes_accessed=1 << 20, transcendentals=0),
    )(*operands)


def tile_kernel(a, b, out):
    for k in range(NY):
        out[k, :UNIT, :] = a[...]
        out[k, UNIT:, :] = b[...]


def join_kernel(a, b, out):
    rows = a.shape[0]
    out[:rows, :] = a[...]
    out[rows:, :] = b[...]


def joined(a, b):
    shape = jax.ShapeDtypeStruct((a.shape[0] + b.shape[0], a.shape[1]), a.dtype)
    return local_call(join_kernel, shape, (a, b))


def half_kernel(line, top, bottom):
    rows = line.shape[1]
    for k in range(NY // 2):
        top[k * rows : (k + 1) * rows, :] = line[k]
        bottom[k * rows : (k + 1) * rows, :] = line[NY // 2 + k]


def gathered(up_shard, down_shard):
    width = up_shard.shape[1]
    h = lambda c: (4 if c == 0 else -4, 0, 0, 0)
    up_other, down_other = fetched(up_shard, h), fetched(down_shard, h)
    tiles = local_call(tile_kernel, jax.ShapeDtypeStruct((NY, 2 * UNIT, width), up_shard.dtype), (up_shard, up_other))
    up_line = lax.all_to_all(tiles, "y", 0, 0, tiled=True)
    half = jax.ShapeDtypeStruct((NY * UNIT, width), up_shard.dtype)
    up_top, up_bottom = local_call(half_kernel, (half, half), (up_line,))

    pair = joined(down_shard, down_other)
    after, before, far = (fetched(pair, along_z(k)) for k in (1, -1, 2))
    return spread(up_top, up_bottom, along_z), spread(joined(pair, after), joined(before, far), along_y)


def up_owners():
    zz = lax.axis_index("z")
    units = []
    for b, half in ((0, 0), (0, 2), (1, 0), (1, 2), (-1, 0), (-1, 2), (2, 0), (-2, 2)):
        for y in (half, half + 1):
            units += [(zz + b + h) % 8 * 4 + y for h in (8, 12)]
    return jnp.stack(units)


def down_owners():
    zz = lax.axis_index("z")
    two = jnp.where(lax.axis_index("c") == 0, 2, -2)
    return jnp.stack([(zz + a + h) % 8 for a in (0, 1, -1, two) for h in (8, 12)])


def up_kernel(table, normed, *refs):
    pieces, (out, scratch) = refs[:8], refs[8:]
    unit = 0
    for piece in pieces:
        for k in range(piece.shape[0] // UNIT):
            to = pl.multiple_of(table[unit] * UNIT, UNIT)
            scratch[pl.ds(to, UNIT), :] = piece[k * UNIT : (k + 1) * UNIT, :]
            unit += 1
    tile = 256
    for n in range(out.shape[1] // tile):
        cols = slice(n * tile, (n + 1) * tile)
        pre = jnp.dot(normed[...], scratch[:, cols], preferred_element_type=jnp.float32)
        out[:, cols] = jnp.square(jnp.maximum(pre, 0.0)).astype(jnp.bfloat16)


def up(table, normed, pieces):
    tokens, width = normed.shape
    hidden = pieces[0].shape[1]
    return local_call(
        up_kernel,
        jax.ShapeDtypeStruct((tokens, hidden), jnp.bfloat16),
        (table, normed, *pieces),
        flops=2 * tokens * width * hidden,
        scratch=[pltpu.VMEM((width, hidden), jnp.bfloat16)],
        tables=1,
        limit=17,
    )


def down_kernel(table, hidden, *refs):
    pieces, out = refs[:-1], refs[-1]
    unit = 0
    for a, b in zip(pieces[::2], pieces[1::2]):
        for piece in (a, b):
            terms = lax.dot_general(piece[...], hidden[...], (((1,), (1,)), ((), ())), preferred_element_type=jnp.float32)
            for k in range(piece.shape[0] // UNIT):
                rows = slice(unit // 8 * UNIT, (unit // 8 + 1) * UNIT)
                out[table[unit % 8], rows, :] = terms[k * UNIT : (k + 1) * UNIT].astype(jnp.bfloat16)
                unit += 1


def down(table, hidden, pieces):
    tokens, depth = hidden.shape
    rows = sum(p.shape[0] for p in pieces)
    return local_call(
        down_kernel,
        jax.ShapeDtypeStruct((8, rows // 8, tokens), jnp.bfloat16),
        (table, hidden, *pieces),
        flops=2 * tokens * depth * rows,
        tables=1,
        limit=12,
    )


def last_kernel(table, own, first, *refs):
    second, (out, scratch) = refs[:4], refs[4:]
    for slot in range(4):
        rows = slice(slot % 2 * UNIT, (slot % 2 + 1) * UNIT)
        parts = [first[k, rows, :] for k in range(4)] if slot < 2 else [ref[rows, :] for ref in second]
        total = sum(part.astype(jnp.float32) for part in parts)
        scratch[pl.ds(pl.multiple_of(table[slot] * UNIT, UNIT), UNIT), :] = total
    out[...] = (own[...].astype(jnp.float32) + scratch[...].T).astype(jnp.bfloat16)


def core_sums(terms):
    arrived = fetched(terms[4:], lambda c: (0, 0, 0, 1))
    return [(terms[k].astype(jnp.float32) + arrived[k].astype(jnp.float32)).astype(jnp.bfloat16) for k in range(4)]


def local(tokens, norm_gain, up_weight, down_weight):
    x, y, c = lax.axis_index("x"), lax.axis_index("y"), lax.axis_index("c")
    up_pieces, down_pieces = gathered(up_weight, down_weight.T)

    xf = tokens.astype(jnp.float32)
    inv_rms = lax.rsqrt(jnp.mean(xf * xf, axis=-1, keepdims=True) + 1e-06)
    normed = (xf * inv_rms * norm_gain).astype(jnp.bfloat16)
    hidden = up(up_owners(), normed, up_pieces)

    owner = down_owners()
    core = jnp.where(owner % 2 == c, 0, 4)
    terms = down(core + owner // 2, hidden, down_pieces[:4])
    sums = core_sums(terms)
    first = lax.all_to_all(jnp.stack(sums), "x", 0, 0, tiled=True)
    terms = down(core + (owner // 2 - x + 4) % 4, hidden, down_pieces[4:])
    sums = core_sums(terms)
    second = [sums[0]] + [fetched(sums[k], lambda c, k=k: (0, 0, -k, 0)) for k in (1, 3, 2)]

    width = tokens.shape[1] // 8
    own = lax.dynamic_slice_in_dim(tokens, (x * 2 + c) * width, width, 1)
    table = jnp.stack([y, (y + 1) % 4, (y + 3) % 4, (y + 2) % 4])
    return local_call(
        last_kernel,
        jax.ShapeDtypeStruct(own.shape, jnp.bfloat16),
        (table, own, first, *second),
        flops=8 * own.size,
        scratch=[pltpu.VMEM(own.shape[::-1], jnp.float32)],
        tables=1,
    )


def solution(mesh):
    torus = Mesh(mesh.devices.reshape(2, 8, NY, NX, NC), AXES)

    return jax.shard_map(
        local,
        mesh=torus,
        in_specs=(P(("r", "z", "y"), None), P(), P(("z", "y"), ("x", "c")), P(("x", "c"), ("z", "y"))),
        out_specs=P(("r", "z", "y"), ("x", "c")),
        check_vma=False,
    )
```

```python
import jax
import jax.numpy as jnp
from jax import lax
from jax.experimental import pallas as pl
from jax.experimental.pallas import tpu as pltpu
from jax.sharding import Mesh
from jax.sharding import PartitionSpec as P


AXES = ("r", "z", "y", "x", "c")
RING, NY, NX, NC = 16, 4, 4, 2
UNIT = 64


def device_number(zz, y, x, c):
    return ((zz % RING * NY + y % NY) * NX + x % NX) * NC + c % NC


def fetched(array, offset):
    pairs = []
    for zz in range(RING):
        for y in range(NY):
            for x in range(NX):
                for c in range(NC):
                    dz, dy, dx, dc = offset(c)
                    pairs.append((device_number(zz + dz, y + dy, x + dx, c + dc), device_number(zz, y, x, c)))
    return lax.ppermute(array, AXES, pairs)


def along_z(k):
    return lambda c: (-k if c else k, 0, 0, 0)


def along_y(k):
    return lambda c: (0, -k if c else k, 0, 0)


def spread(top, bottom, step):
    next_top, before_bottom = fetched(top, step(1)), fetched(bottom, step(-1))
    next_bottom, before_top = fetched(bottom, step(1)), fetched(top, step(-1))
    far_top, far_bottom = fetched(next_top, step(1)), fetched(before_bottom, step(-1))
    return top, bottom, next_top, next_bottom, before_top, before_bottom, far_top, far_bottom


VMEM = pl.BlockSpec(memory_space=pltpu.VMEM)
SMEM = pl.BlockSpec(memory_space=pltpu.SMEM)


def local_call(kernel, shapes, operands, flops=0, scratch=(), tables=0, limit=8):
    return pl.pallas_call(
        kernel,
        out_shape=shapes,
        in_specs=[SMEM] * tables + [VMEM] * (len(operands) - tables),
        out_specs=jax.tree.map(lambda _: VMEM, shapes),
        scratch_shapes=list(scratch),
        compiler_params=pltpu.CompilerParams(vmem_limit_bytes=limit << 20),
        cost_estimate=pl.CostEstimate(flops=flops, bytes_accessed=1 << 20, transcendentals=0),
    )(*operands)


def tile_kernel(a, b, out):
    for k in range(NY):
        out[k, :UNIT, :] = a[...]
        out[k, UNIT:, :] = b[...]


def join_kernel(*refs):
    out, row = refs[-1], 0
    for part in refs[:-1]:
        out[row : row + part.shape[0], :] = part[...]
        row += part.shape[0]


def joined(parts):
    shape = jax.ShapeDtypeStruct((sum(p.shape[0] for p in parts), parts[0].shape[1]), parts[0].dtype)
    return local_call(join_kernel, shape, parts)


def half_kernel(line, top, bottom):
    rows = line.shape[1]
    for k in range(NY // 2):
        top[k * rows : (k + 1) * rows, :] = line[k]
        bottom[k * rows : (k + 1) * rows, :] = line[NY // 2 + k]


def gathered(up_shard, down_shard):
    width = up_shard.shape[1]
    h = lambda c: (4 if c == 0 else -4, 0, 0, 0)
    up_other, down_other = fetched(up_shard, h), fetched(down_shard, h)
    tiles = local_call(tile_kernel, jax.ShapeDtypeStruct((NY, 2 * UNIT, width), up_shard.dtype), (up_shard, up_other))
    up_line = lax.all_to_all(tiles, "y", 0, 0, tiled=True)
    half = jax.ShapeDtypeStruct((NY * UNIT, width), up_shard.dtype)
    up_top, up_bottom = local_call(half_kernel, (half, half), (up_line,))

    pair = joined((down_shard, down_other))
    line = joined((pair, *(fetched(pair, along_z(k)) for k in (1, -1, 2))))
    after, before = fetched(line, along_y(1)), fetched(line, along_y(-1))
    half = line.shape[0] // 2
    far = fetched(after[:half], along_y(1)), fetched(before[half:], along_y(-1))
    return spread(up_top, up_bottom, along_z), (line, after, before), far


def up_owners(way):
    zz = lax.axis_index("z")
    units = []
    for b, half in ((0, 0), (0, 2), (1, 0), (1, 2), (-1, 0), (-1, 2), (2, 0), (-2, 2)):
        for y in (half, half + 1):
            units += [(zz + way * b + h) % 8 * 4 + y for h in (8, 12)]
    return jnp.stack(units)


def down_owners(way):
    zz = lax.axis_index("z")
    return jnp.stack([(zz + way * a + h) % 8 for a in (0, 1, -1, 2) for h in (8, 12)])


def up_kernel(table, normed, *refs):
    pieces, (out, scratch) = refs[:8], refs[8:]
    unit = 0
    for piece in pieces:
        for k in range(piece.shape[0] // UNIT):
            to = pl.multiple_of(table[unit] * UNIT, UNIT)
            scratch[pl.ds(to, UNIT), :] = piece[k * UNIT : (k + 1) * UNIT, :]
            unit += 1
    tile = 256
    for n in range(out.shape[1] // tile):
        cols = slice(n * tile, (n + 1) * tile)
        pre = jnp.dot(normed[...], scratch[:, cols], preferred_element_type=jnp.float32)
        out[:, cols] = jnp.square(jnp.maximum(pre, 0.0)).astype(jnp.bfloat16)


def up(table, normed, pieces):
    tokens, width = normed.shape
    hidden = pieces[0].shape[1]
    return local_call(
        up_kernel,
        jax.ShapeDtypeStruct((tokens, hidden), jnp.bfloat16),
        (table, normed, *pieces),
        flops=2 * tokens * width * hidden,
        scratch=[pltpu.VMEM((width, hidden), jnp.bfloat16)],
        tables=1,
        limit=17,
    )


def down_kernel(table, hidden, *refs):
    pieces, out = refs[:-1], refs[-1]
    unit = 0
    for piece in pieces:
        terms = lax.dot_general(piece[...], hidden[...], (((1,), (1,)), ((), ())), preferred_element_type=jnp.float32)
        for k in range(piece.shape[0] // UNIT):
            rows = pl.ds(pl.multiple_of(table[8 + unit // 8] * UNIT, UNIT), UNIT)
            out[table[unit % 8], rows, :] = terms[k * UNIT : (k + 1) * UNIT].astype(jnp.bfloat16)
            unit += 1


def down(table, hidden, pieces):
    tokens, depth = hidden.shape
    rows = sum(p.shape[0] for p in pieces)
    return local_call(
        down_kernel,
        jax.ShapeDtypeStruct((8, rows // 8, tokens), jnp.bfloat16),
        (table, hidden, *pieces),
        flops=2 * tokens * depth * rows,
        tables=1,
        limit=12,
    )


def last_kernel(table, own, near, *refs):
    far, (out, scratch) = refs[:4], refs[4:]
    for slot in range(4):
        parts = [near[k, slot * UNIT : (slot + 1) * UNIT, :] for k in range(4)] if slot < 3 else [ref[...] for ref in far]
        total = sum(part.astype(jnp.float32) for part in parts)
        scratch[pl.ds(pl.multiple_of(table[slot] * UNIT, UNIT), UNIT), :] = total
    out[...] = (own[...].astype(jnp.float32) + scratch[...].T).astype(jnp.bfloat16)


def arrived(terms):
    return fetched(terms[4:], lambda c: (0, 0, 0, 1)).astype(jnp.float32)


def local(tokens, norm_gain, up_weight, down_weight):
    x, y, c = lax.axis_index("x"), lax.axis_index("y"), lax.axis_index("c")
    way = 1 - 2 * c
    up_pieces, near, far = gathered(up_weight, down_weight.T)

    xf = tokens.astype(jnp.float32)
    inv_rms = lax.rsqrt(jnp.mean(xf * xf, axis=-1, keepdims=True) + 1e-06)
    normed = (xf * inv_rms * norm_gain).astype(jnp.bfloat16)
    hidden = up(up_owners(way), normed, up_pieces)

    owner = down_owners(way)
    mine = owner % 2 == c
    slots = jnp.stack([0 * c, 1 + c, 2 - c])
    terms = down(jnp.concatenate([jnp.where(mine, 0, 4) + owner // 2, slots]), hidden, near)
    sums = (terms[:4].astype(jnp.float32) + arrived(terms)).astype(jnp.bfloat16)
    near = lax.all_to_all(sums, "x", 0, 0, tiled=True)
    ahead = owner // 2 - x
    places = jnp.where(mine, (way * ahead + 4) % 4, 4 + (4 - way * ahead) % 4)
    terms = down(jnp.concatenate([places, slots]), hidden, far)
    other = arrived(terms)
    sums = [(terms[k].astype(jnp.float32) + other[k]).astype(jnp.bfloat16) for k in range(4)]
    far = [sums[0]] + [fetched(sums[k], lambda c, k=k: (0, 0, k if c else -k, 0)) for k in (1, 3, 2)]

    width = tokens.shape[1] // 8
    own = lax.dynamic_slice_in_dim(tokens, (x * 2 + c) * width, width, 1)
    table = jnp.stack([y, (y + 1) % 4, (y + 3) % 4, (y + 2) % 4])
    return local_call(
        last_kernel,
        jax.ShapeDtypeStruct(own.shape, jnp.bfloat16),
        (table, own, near, *far),
        flops=8 * own.size,
        scratch=[pltpu.VMEM(own.shape[::-1], jnp.float32)],
        tables=1,
    )


def solution(mesh):
    torus = Mesh(mesh.devices.reshape(2, 8, NY, NX, NC), AXES)

    return jax.shard_map(
        local,
        mesh=torus,
        in_specs=(P(("r", "z", "y"), None), P(), P(("z", "y"), ("x", "c")), P(("x", "c"), ("z", "y"))),
        out_specs=P(("r", "z", "y"), ("x", "c")),
        check_vma=False,
    )
```
